32 devices in a mesh: rep: 8 (over z, y), fs: 2 (over x), tp: 2 (over core).
Axes of the slice: x: 2, y: 2, z: 4, core: 2. Of those that a mesh axis runs over, the one named last changes fastest.
Arguments:
- tokens: bfloat16 [8192, 1024], P(('rep', 'fs', 'tp')), may hold values from -6 to 6
- cotangent: bfloat16 [8192, 1024], P(('rep', 'fs', 'tp')), may hold values from -8 to 8
- gate_weight: bfloat16 [1024, 2816], P(None, ('fs', 'tp')), may hold values from -0.1875 to 0.1875
- value_weight: bfloat16 [1024, 2816], P(None, ('fs', 'tp')), may hold values from -0.1875 to 0.1875
- down_weight: bfloat16 [2816, 1024], P(('fs', 'tp')), may hold values from -0.109375 to 0.109375
- gate_taps: float32 [3, 2816], P(None, ('fs', 'tp')), may hold values from -3.5 to 3.5
- value_taps: float32 [3, 2816], P(None, ('fs', 'tp')), may hold values from -3.5 to 3.5
Outputs:
- input_grad: bfloat16 [8192, 1024], P(('rep', 'fs', 'tp'))
- gate_grad: float32 [1024, 2816], P(None, ('fs', 'tp'))
- value_grad: float32 [1024, 2816], P(None, ('fs', 'tp'))
- down_grad: float32 [2816, 1024], P(('fs', 'tp'))
- gate_taps_grad: float32 [3, 2816], P(None, ('fs', 'tp'))
- value_taps_grad: float32 [3, 2816], P(None, ('fs', 'tp'))
The draws below stay inside these ranges and needn't reach their ends.
All inputs are finite; a program needn't handle non-finite values.
Results may differ from the reference program's by a relative error of at most 0.0062.
Values may be sent and summed in bfloat16 or wider, within the bound.
No kernel may reach another device: no remote copies, remote signals or barrier semaphores. Data moves between devices by JAX's collectives and lax.ppermute only.
A program may use at most 128 MiB of HBM per device.

```python
import jax
import jax.numpy as jnp
from jax import lax

D = 1024
FF = 2816
TAPS = 3
SEQ = 1024
TOKENS = 8192
N_REP = 8


def strengthened(entries, own_key, source, target, blocks, factor):
    def block_of(dim):
        return (jnp.arange(entries.shape[dim]) // (entries.shape[dim] // blocks)).reshape((-1,) + (1,) * (entries.ndim - 1 - dim))

    first = jax.random.permutation(own_key, blocks)[block_of(target)]
    other_side = (block_of(target) + blocks // 2) % blocks
    return jnp.where((block_of(source) == first) | (block_of(source) == other_side), factor * entries, entries)


def steps_of(stream_key, shape, cuts, least, high):
    level = 1.0
    for axis_at, blocks in cuts:
        draws = jax.random.uniform(jax.random.fold_in(jax.random.fold_in(stream_key, 6), axis_at), (blocks,), jnp.float32, least / len(cuts), high / len(cuts))
        level = level * jnp.repeat(jnp.exp(draws), shape[axis_at] // blocks).reshape((-1,) + (1,) * (len(shape) - 1 - axis_at))
    return level


def centred(stream_key, dims, deviation, reach, cuts=(), dtype=jnp.bfloat16):
    entries = deviation * jax.random.normal(stream_key, dims, jnp.float32)
    if cuts:
        entries = entries * steps_of(stream_key, dims, cuts, -0.22, 0.18)
    return jnp.clip(entries, -reach, reach).astype(dtype)


def heavy_noise(own_key, dims, width, limit, pieces, heavy, held_as=jnp.bfloat16):
    entries = width * jax.random.normal(own_key, dims, jnp.float32)
    if pieces:
        entries = entries * steps_of(own_key, dims, pieces, -0.22, 0.18)
    return jnp.clip(strengthened(entries, jax.random.fold_in(own_key, 3), *heavy), -limit, limit).astype(held_as)


def setup_inputs(seed: int = 0) -> dict:
    keys = jax.random.split(jax.random.key(seed), 8)
    tokens = centred(keys[0], (TOKENS, D), 1.0, 6.0, ((0, 32),))
    cotangent = heavy_noise(keys[1], (TOKENS, D), 1.0, 8.0, ((0, 32),), (0, 1, 32, 2.75))
    gate_weight = centred(keys[2], (D, FF), D ** -0.5, 0.1875, ((1, 4),))
    value_weight = centred(keys[3], (D, FF), D ** -0.5, 0.1875, ((1, 4),))
    down_weight = centred(keys[4], (FF, D), FF ** -0.5, 0.109375, ((0, 4),))
    gate_taps = centred(keys[5], (TAPS, FF), TAPS ** -0.5, 3.5, ((1, 4),), jnp.float32)
    value_taps = centred(keys[6], (TAPS, FF), TAPS ** -0.5, 3.5, ((1, 4),), jnp.float32)
    return {"tokens": tokens, "cotangent": cotangent, "gate_weight": gate_weight, "value_weight": value_weight, "down_weight": down_weight, "gate_taps": gate_taps, "value_taps": value_taps}


def shift_back(field, offset):
    return jnp.pad(field, ((offset, 0), (0, 0)))[:field.shape[0]]


def shift_ahead(field, offset):
    return jnp.pad(field, ((0, offset), (0, 0)))[offset:]


def causal_mix(field, taps):
    total = taps[0][None, :] * field
    for offset in range(1, TAPS):
        total = total + taps[offset][None, :] * shift_back(field, offset)
    return total


def reverse_mix(field, taps):
    total = taps[0][None, :] * field
    for offset in range(1, TAPS):
        total = total + taps[offset][None, :] * shift_ahead(field, offset)
    return total


def tap_sums(back, field):
    return jnp.stack([jnp.sum(back * shift_back(field, offset), axis=0) for offset in range(TAPS)])


def contract_rows(left, right):
    return lax.dot_general(left, right, (((0,), (0,)), ((), ())), preferred_element_type=jnp.float32)


def contract_cols(left, right):
    return lax.dot_general(left, right, (((1,), (1,)), ((), ())), preferred_element_type=jnp.float32)


def reference(tokens, cotangent, gate_weight, value_weight, down_weight, gate_taps, value_taps):
    rows_all = tokens.reshape(N_REP, SEQ, D)
    cots_all = cotangent.reshape(N_REP, SEQ, D)

    def one_sequence(carry, pair):
        rows, cots = pair
        up_gate = lax.optimization_barrier(jnp.dot(rows, gate_weight, preferred_element_type=jnp.float32).astype(jnp.bfloat16)).astype(jnp.float32)
        up_value = lax.optimization_barrier(jnp.dot(rows, value_weight, preferred_element_type=jnp.float32).astype(jnp.bfloat16)).astype(jnp.float32)
        conv_gate = causal_mix(up_gate, gate_taps)
        conv_value = causal_mix(up_value, value_taps)
        sigma = jax.nn.sigmoid(conv_gate)
        silu_gate = conv_gate * sigma
        hidden = (silu_gate * conv_value).astype(jnp.bfloat16)
        back_hidden = contract_cols(cots, down_weight)
        back_value = back_hidden * silu_gate
        back_gate = back_hidden * conv_value * sigma * (1.0 + conv_gate * (1.0 - sigma))
        grad_gate = reverse_mix(back_gate, gate_taps).astype(jnp.bfloat16)
        grad_value = reverse_mix(back_value, value_taps).astype(jnp.bfloat16)
        input_grad = (contract_cols(grad_gate, gate_weight) + contract_cols(grad_value, value_weight)).astype(jnp.bfloat16)
        new_carry = (carry[0] + contract_rows(rows, grad_gate),
                     carry[1] + contract_rows(rows, grad_value),
                     carry[2] + contract_rows(hidden, cots),
                     carry[3] + tap_sums(back_gate, up_gate),
                     carry[4] + tap_sums(back_value, up_value))
        return new_carry, input_grad

    start = (jnp.zeros((D, FF), jnp.float32), jnp.zeros((D, FF), jnp.float32),
             jnp.zeros((FF, D), jnp.float32), jnp.zeros((TAPS, FF), jnp.float32),
             jnp.zeros((TAPS, FF), jnp.float32))
    sums, grads = lax.scan(one_sequence, start, (rows_all, cots_all))
    scale = TOKENS ** -0.5
    return (grads.reshape(TOKENS, D), sums[0] * scale, sums[1] * scale, sums[2] * scale,
            sums[3] * scale, sums[4] * scale)
```

```python
import functools
import math

import jax
import jax.numpy as jnp
from jax import lax
from jax.experimental import pallas as pl
from jax.experimental.pallas import tpu as pltpu
from jax.sharding import PartitionSpec as P


F32 = jnp.float32
BF16 = jnp.bfloat16
LANES = 128
GROUP = 32


def bit_count(size):
    return size.bit_length() - 1


def exchange(value, axis, bit):
    size = lax.axis_size(axis)
    return lax.ppermute(value, axis, [(i, i ^ (1 << bit)) for i in range(size)])


def col_tiles(width):
    return [(start, min(start + LANES, width)) for start in range(0, width, LANES)]


def forward_kernel(me_ref, gate_ref, value_ref, gtaps_ref, vtaps_ref, hidden_ref, silu_ref, slope_ref, gcarry, vcarry):
    step = pl.program_id(0)
    rows, width = gate_ref.shape[1:]
    count = gtaps_ref.shape[0]

    @pl.when(step == 0)
    def _():
        gcarry[...] = jnp.zeros_like(gcarry)
        vcarry[...] = jnp.zeros_like(vcarry)

    for lo, hi in col_tiles(width):
        gtaps = [gtaps_ref[k : k + 1, lo:hi] for k in range(count)]
        vtaps = [vtaps_ref[k : k + 1, lo:hi] for k in range(count)]

        def mixed(carry, block, taps):
            ext = jnp.concatenate([carry, block], axis=0)
            total = taps[0] * block
            for k in range(1, count):
                total = total + taps[k] * ext[8 - k : 8 - k + GROUP]
            return total, block[GROUP - 8 :]

        def body(i, carry):
            at = pl.ds(pl.multiple_of(i * GROUP, GROUP), GROUP)
            gate, gnext = mixed(carry[0], gate_ref[0, at, lo:hi].astype(F32), gtaps)
            value, vnext = mixed(carry[1], value_ref[0, at, lo:hi].astype(F32), vtaps)
            sigma = jax.nn.sigmoid(gate)
            silu = gate * sigma
            hidden_ref[0, at, lo:hi] = (silu * value).astype(hidden_ref.dtype)
            silu_ref[0, at, lo:hi] = silu
            slope_ref[0, at, lo:hi] = value * sigma * (1.0 + gate * (1.0 - sigma))
            return gnext, vnext

        gout, vout = lax.fori_loop(0, rows // GROUP, body, (gcarry[:, lo:hi], vcarry[:, lo:hi]))
        gcarry[:, lo:hi] = gout
        vcarry[:, lo:hi] = vout


def forward_part(me, gate, value, gtaps, vtaps):
    blocks, rows, width = gate.shape
    block = pl.BlockSpec((1, rows, width), lambda q, me_ref: (q ^ me_ref[0], 0, 0))
    taps = pl.BlockSpec(gtaps.shape, lambda q, me_ref: (0, 0))
    shape = (blocks, rows, width)
    return pl.pallas_call(
        forward_kernel,
        out_shape=(
            jax.ShapeDtypeStruct(shape, BF16),
            jax.ShapeDtypeStruct(shape, F32),
            jax.ShapeDtypeStruct(shape, F32),
        ),
        grid_spec=pltpu.PrefetchScalarGridSpec(
            num_scalar_prefetch=1,
            grid=(blocks,),
            in_specs=[block, block, taps, taps],
            out_specs=(block, block, block),
            scratch_shapes=[pltpu.VMEM((8, width), F32), pltpu.VMEM((8, width), F32)],
        ),
        compiler_params=pltpu.CompilerParams(dimension_semantics=("arbitrary",)),
        cost_estimate=pl.CostEstimate(flops=40 * blocks * rows * width, bytes_accessed=14 * blocks * rows * width, transcendentals=2 * blocks * rows * width),
        name="forward_part",
    )(me, gate, value, gtaps, vtaps)


def backward_kernel(
    me_ref, cot_ref, down_ref, silu_ref, slope_ref, gate_ref, value_ref, gtaps_ref, vtaps_ref,
    ggrad_ref, vgrad_ref, sums_ref, back, gcarry, vcarry,
):
    step = pl.program_id(0)
    rows, width = gate_ref.shape[1:]
    count = gtaps_ref.shape[0]
    groups = rows // GROUP

    @pl.when(step == 0)
    def _():
        gcarry[...] = jnp.zeros_like(gcarry)
        vcarry[...] = jnp.zeros_like(vcarry)
        sums_ref[...] = jnp.zeros_like(sums_ref)

    back[...] = lax.dot_general(
        cot_ref[0], down_ref[...], (((1,), (1,)), ((), ())), preferred_element_type=F32
    )
    for lo, hi in col_tiles(width):
        gtaps = [gtaps_ref[k : k + 1, lo:hi] for k in range(count)]
        vtaps = [vtaps_ref[k : k + 1, lo:hi] for k in range(count)]

        def mixed(carry, block, field, taps, sums):
            ext = jnp.concatenate([block, carry], axis=0)
            total = taps[0] * block
            out = []
            for k in range(count):
                moved = block if k == 0 else ext[k : k + GROUP]
                if k:
                    total = total + taps[k] * moved
                out.append(sums[k] + jnp.sum((moved * field).reshape(GROUP // 8, 8, hi - lo), axis=0))
            return total, block[:8], out

        def body(i, carry):
            gnext, vnext, gsums, vsums = carry
            at = pl.ds(pl.multiple_of((groups - 1 - i) * GROUP, GROUP), GROUP)
            up = back[at, lo:hi]
            gback = up * slope_ref[0, at, lo:hi]
            vback = up * silu_ref[0, at, lo:hi]
            gate, gnext, gsums = mixed(gnext, gback, gate_ref[0, at, lo:hi].astype(F32), gtaps, gsums)
            value, vnext, vsums = mixed(vnext, vback, value_ref[0, at, lo:hi].astype(F32), vtaps, vsums)
            ggrad_ref[0, at, lo:hi] = gate.astype(ggrad_ref.dtype)
            vgrad_ref[0, at, lo:hi] = value.astype(vgrad_ref.dtype)
            return gnext, vnext, gsums, vsums

        zeros = [jnp.zeros((8, hi - lo), F32) for _ in range(count)]
        gout, vout, gsums, vsums = lax.fori_loop(
            0, groups, body, (gcarry[:, lo:hi], vcarry[:, lo:hi], zeros, zeros)
        )
        gcarry[:, lo:hi] = gout
        vcarry[:, lo:hi] = vout
        for k in range(count):
            sums_ref[k : k + 1, lo:hi] += jnp.sum(gsums[k], axis=0, keepdims=True)
            sums_ref[count + k : count + k + 1, lo:hi] += jnp.sum(vsums[k], axis=0, keepdims=True)


def backward_part(me, cot, down, silu, slope, gate, value, gtaps, vtaps):
    blocks, rows, width = gate.shape
    model = down.shape[1]
    last = blocks - 1
    block = pl.BlockSpec((1, rows, width), lambda q, me_ref: ((last - q) ^ me_ref[0], 0, 0))
    taps = pl.BlockSpec(gtaps.shape, lambda q, me_ref: (0, 0))
    sums = (2 * gtaps.shape[0], width)
    shape = (blocks, rows, width)
    return pl.pallas_call(
        backward_kernel,
        out_shape=(
            jax.ShapeDtypeStruct(shape, BF16),
            jax.ShapeDtypeStruct(shape, BF16),
            jax.ShapeDtypeStruct(sums, F32),
        ),
        grid_spec=pltpu.PrefetchScalarGridSpec(
            num_scalar_prefetch=1,
            grid=(blocks,),
            in_specs=[
                pl.BlockSpec((1, rows, model), lambda q, me_ref: ((last - q) ^ me_ref[0], 0, 0)),
                pl.BlockSpec(down.shape, lambda q, me_ref: (0, 0)),
                block, block, block, block, taps, taps,
            ],
            out_specs=(block, block, pl.BlockSpec(sums, lambda q, me_ref: (0, 0))),
            scratch_shapes=[
                pltpu.VMEM((rows, width), F32),
                pltpu.VMEM((8, width), F32),
                pltpu.VMEM((8, width), F32),
            ],
        ),
        compiler_params=pltpu.CompilerParams(dimension_semantics=("arbitrary",)),
        cost_estimate=pl.CostEstimate(flops=2 * blocks * rows * width * model, bytes_accessed=16 * blocks * rows * width, transcendentals=0),
        name="backward_part",
    )(me, cot, down, silu, slope, gate, value, gtaps, vtaps)


def rows_kernel(where_ref, left_ref, right_ref, out_ref):
    half = out_ref.shape[1]
    full = lax.dot_general(
        left_ref[...], right_ref[...], (((0,), (0,)), ((), ())), preferred_element_type=F32
    ).astype(out_ref.dtype)
    swap = where_ref[1]
    out_ref[swap] = full[:half]
    out_ref[1 - swap] = full[half:]


def rows_product(where, left, right, blocks):
    tokens, model = left.shape
    width = right.shape[1]
    size = model // blocks
    return pl.pallas_call(
        rows_kernel,
        out_shape=jax.ShapeDtypeStruct((2, size // 2, width), BF16),
        grid_spec=pltpu.PrefetchScalarGridSpec(
            num_scalar_prefetch=1,
            grid=(1,),
            in_specs=[
                pl.BlockSpec((tokens, size), lambda i, where_ref: (0, where_ref[0])),
                pl.BlockSpec((tokens, width), lambda i, where_ref: (0, 0)),
            ],
            out_specs=pl.BlockSpec((2, size // 2, width), lambda i, where_ref: (0, 0, 0)),
        ),
        cost_estimate=pl.CostEstimate(flops=2 * tokens * size * width, bytes_accessed=2 * (tokens * size + tokens * width + size * width), transcendentals=0),
        name="rows_product",
    )(where, left, right)


def cols_kernel(where_ref, left_ref, right_ref, out_ref):
    half = out_ref.shape[2]
    full = lax.dot_general(
        left_ref[...], right_ref[...], (((0,), (0,)), ((), ())), preferred_element_type=F32
    ).astype(out_ref.dtype)
    swap = where_ref[1]
    out_ref[swap] = full[:, :half]
    out_ref[1 - swap] = full[:, half:]


def cols_product(where, left, right, blocks):
    tokens, width = left.shape
    size = right.shape[1] // blocks
    return pl.pallas_call(
        cols_kernel,
        out_shape=jax.ShapeDtypeStruct((2, width, size // 2), BF16),
        grid_spec=pltpu.PrefetchScalarGridSpec(
            num_scalar_prefetch=1,
            grid=(1,),
            in_specs=[
                pl.BlockSpec((tokens, width), lambda i, where_ref: (0, 0)),
                pl.BlockSpec((tokens, size), lambda i, where_ref: (0, where_ref[0])),
            ],
            out_specs=pl.BlockSpec((2, width, size // 2), lambda i, where_ref: (0, 0, 0)),
        ),
        cost_estimate=pl.CostEstimate(flops=2 * tokens * size * width, bytes_accessed=2 * (tokens * size + tokens * width + size * width), transcendentals=0),
        name="cols_product",
    )(where, left, right)


def add(left, right, dtype):
    return (left.astype(F32) + right.astype(F32)).astype(dtype)


def rep_bit(bit):
    return (lax.axis_index("rep") >> bit) & 1


def reduce_chunk(product, color, colors, first, second):
    mine_first, mine_second = rep_bit(first), rep_bit(second)
    sent = product(jnp.stack([2 * color + 1 - mine_first, mine_second]), 2 * colors)
    got = exchange(sent, "rep", first)
    kept = product(jnp.stack([2 * color + mine_first, mine_second]), 2 * colors)
    over = exchange(add(kept[1], got[1], BF16), "rep", second)
    mine = add(add(kept[0], got[0], F32), over, BF16)
    rest = [b for b in range(bit_count(lax.axis_size("rep"))) if b not in (first, second)]
    for at, bit in enumerate(rest):
        theirs = exchange(mine, "rep", bit)
        mine = add(mine, theirs, BF16 if at == len(rest) - 1 else F32)
    other = exchange(mine, "rep", second)
    pair = jnp.stack([mine, other])
    return pair, exchange(pair, "rep", first)


def place_rows_kernel(scale, where_ref, *refs):
    out_ref = refs[-1]
    step = pl.program_id(0)
    for at, ref in enumerate(refs[:-1]):
        for i in range(2):

            @pl.when(step == 2 * at + i)
            def _(ref=ref, i=i):
                out_ref[...] = ref[i].astype(F32) * scale


def place(parts, spots, scale, rows):
    height, width = parts[0].shape[1:]
    steps = 2 * len(parts)
    if rows:
        out = (steps * height, width)
        spec = pl.BlockSpec((height, width), lambda i, where_ref: (where_ref[i], 0))
    else:
        out = (height, steps * width)
        spec = pl.BlockSpec((height, width), lambda i, where_ref: (0, where_ref[i]))
    whole = pl.BlockSpec(parts[0].shape, lambda i, where_ref: (0, 0, 0))
    return pl.pallas_call(
        functools.partial(place_rows_kernel, scale),
        out_shape=jax.ShapeDtypeStruct(out, F32),
        grid_spec=pltpu.PrefetchScalarGridSpec(
            num_scalar_prefetch=1, grid=(steps,), in_specs=[whole] * len(parts), out_specs=spec
        ),
        compiler_params=pltpu.CompilerParams(dimension_semantics=("arbitrary",)),
        cost_estimate=pl.CostEstimate(flops=out[0] * out[1], bytes_accessed=6 * out[0] * out[1], transcendentals=0),
        name="place",
    )(spots, *parts)


def spots_of(color, first, second):
    flip = 2 * rep_bit(first) + rep_bit(second)
    return 4 * color + (jnp.arange(4, dtype=jnp.int32) ^ flip)


ORDERS = ((0, 1), (1, 0))


def sum_over_rep(product, scale, rows):
    parts, spots = [], []
    for color, (first, second) in enumerate(ORDERS):
        parts.extend(reduce_chunk(product, color, len(ORDERS), first, second))
        spots.append(spots_of(color, first, second))
    return place(parts, jnp.concatenate(spots), scale, rows)


def butterfly(value):
    for bit in range(bit_count(lax.axis_size("rep"))):
        value = value + exchange(value, "rep", bit)
    return value


def gather_relative(own):
    found = [own]
    for axis in ("tp", "fs"):
        for bit in range(bit_count(lax.axis_size(axis))):
            found = found + [exchange(item, axis, bit) for item in found]
    return jnp.concatenate(found, axis=0)


def scatter_relative(blocks):
    count = blocks.shape[0]
    for axis in ("fs", "tp")[::-1]:
        pass
    bits = [("tp", b) for b in range(bit_count(lax.axis_size("tp")))]
    bits += [("fs", b) for b in range(bit_count(lax.axis_size("fs")))]
    pending = {r: blocks[r] for r in range(count)}
    for at, (axis, bit) in enumerate(bits):
        sent = [r for r in pending if (r >> at) & 1]
        moved = exchange(jnp.stack([pending[r] for r in sent]).astype(BF16), axis, bit)
        pending = {r ^ (1 << at): pending[r ^ (1 << at)].astype(F32) + moved[i].astype(F32) for i, r in enumerate(sent)}
    return pending[0]


def per_device(tokens, cotangent, gate_weight, value_weight, down_weight, gate_taps, value_taps):
    rows, model = tokens.shape
    width = gate_weight.shape[1]
    parts = lax.axis_size("fs") * lax.axis_size("tp")
    scale = 1.0 / math.sqrt(rows * parts * lax.axis_size("rep"))
    me = (lax.axis_index("fs") * lax.axis_size("tp") + lax.axis_index("tp")).astype(jnp.int32)[None]

    whole = gather_relative(tokens)
    cots = gather_relative(cotangent)
    up_gate = jnp.dot(whole, gate_weight, preferred_element_type=F32).astype(BF16).reshape(parts, rows, width)
    up_value = jnp.dot(whole, value_weight, preferred_element_type=F32).astype(BF16).reshape(parts, rows, width)
    hidden, silu, slope = forward_part(me, up_gate, up_value, gate_taps, value_taps)
    hidden = hidden.reshape(parts * rows, width)
    down = sum_over_rep(lambda where, blocks: cols_product(where, hidden, cots, blocks), scale, False)
    ggrad, vgrad, sums = backward_part(
        me, cots.reshape(parts, rows, model), down_weight, silu, slope, up_gate, up_value, gate_taps, value_taps
    )
    ggrad = ggrad.reshape(parts * rows, width)
    vgrad = vgrad.reshape(parts * rows, width)
    value = sum_over_rep(lambda where, blocks: rows_product(where, whole, vgrad, blocks), scale, True)
    gate = sum_over_rep(lambda where, blocks: rows_product(where, whole, ggrad, blocks), scale, True)
    sums = butterfly(sums) * scale
    partial = lax.dot_general(ggrad, gate_weight, (((1,), (1,)), ((), ())), preferred_element_type=F32)
    partial = partial + lax.dot_general(vgrad, value_weight, (((1,), (1,)), ((), ())), preferred_element_type=F32)
    input_grad = scatter_relative(partial.reshape(parts, rows, model)).astype(BF16)
    count = gate_taps.shape[0]
    return input_grad, gate, value, down, sums[:count], sums[count:]


def solution(mesh):
    in_specs = (
        P(("rep", "fs", "tp"), None),
        P(("rep", "fs", "tp"), None),
        P(None, ("fs", "tp")),
        P(None, ("fs", "tp")),
        P(("fs", "tp"), None),
        P(None, ("fs", "tp")),
        P(None, ("fs", "tp")),
    )
    out_specs = (
        P(("rep", "fs", "tp"), None),
        P(None, ("fs", "tp")),
        P(None, ("fs", "tp")),
        P(("fs", "tp"), None),
        P(None, ("fs", "tp")),
        P(None, ("fs", "tp")),
    )
    return jax.shard_map(
        per_device, mesh=mesh, in_specs=in_specs, out_specs=out_specs, check_vma=False
    )
```

```python
import functools
import math

import jax
import jax.numpy as jnp
from jax import lax
from jax.experimental import pallas as pl
from jax.experimental.pallas import tpu as pltpu
from jax.sharding import PartitionSpec as P


F32 = jnp.float32
BF16 = jnp.bfloat16
LANES = 128
SUBLANES = 8
CHUNKS = 4
CALLS = 2
LIMIT = 60000 * 2**10
ORDERS = ((0, 1), (1, 0), (0, 1), (1, 0))
UNROLL = 1


def bit_count(size):
    return size.bit_length() - 1


def exchange(value, axis, bit):
    size = lax.axis_size(axis)
    return lax.ppermute(value, axis, [(i, i ^ (1 << bit)) for i in range(size)])


FINISH = (0, 1, 3, 2)


def rep_bit(bit):
    return (lax.axis_index("rep") >> bit) & 1


def dot_rows(left, right):
    return lax.dot_general(left, right, (((1,), (1,)), ((), ())), preferred_element_type=F32)


def dot(left, right):
    return lax.dot_general(left, right, (((1,), (0,)), ((), ())), preferred_element_type=F32)


def lane_index():
    return lax.broadcasted_iota(jnp.int32, (SUBLANES, LANES), 1)


def moved_later(tiles, offset):
    lane = lane_index()
    turned = [pltpu.roll(tile, offset, 1) for tile in tiles]
    before = [jnp.zeros_like(tiles[0])] + turned[:-1]
    return [jnp.where(lane < offset, b, t) for b, t in zip(before, turned)]


def moved_earlier(tiles, offset):
    lane = lane_index()
    turned = [pltpu.roll(tile, LANES - offset, 1) for tile in tiles]
    after = turned[1:] + [jnp.zeros_like(tiles[0])]
    return [jnp.where(lane >= LANES - offset, a, t) for a, t in zip(after, turned)]


def load_tiles(ref, at):
    return [ref[at, i : i + LANES] for i in range(0, ref.shape[1], LANES)]


def forward_kernel(parts, me_ref, *refs):
    pieces = refs[:parts]
    gate_ref, value_ref, gtaps_ref, vtaps_ref = refs[parts : parts + 4]
    hidden_ref, silu_ref, slope_ref, upg_ref, upv_ref = refs[parts + 4 :]
    height = gate_ref.shape[0]
    rows = pieces[0].shape[0]
    count = gtaps_ref.shape[1]
    weights = jnp.concatenate([gate_ref[...], value_ref[...]], axis=0)
    for r, piece in enumerate(pieces):
        at = pl.ds(pl.multiple_of((me_ref[0] ^ r) * rows, rows), rows)
        up = dot_rows(weights, piece[...]).astype(BF16)
        upg_ref[:, at] = up[:height]
        upv_ref[:, at] = up[height:]

    def mixed(tiles, taps_ref, at):
        total = None
        for k in range(count):
            tap = jnp.broadcast_to(taps_ref[at, k : k + 1], (SUBLANES, LANES))
            terms = [tap * tile for tile in (moved_later(tiles, k) if k else tiles)]
            total = terms if total is None else [a + b for a, b in zip(total, terms)]
        return total

    def body(i, carry):
        both = pl.ds(pl.multiple_of(i * 2 * SUBLANES, 2 * SUBLANES), 2 * SUBLANES)
        upg = [tile.astype(F32) for tile in load_tiles(upg_ref, both)]
        upv = [tile.astype(F32) for tile in load_tiles(upv_ref, both)]
        halves = []
        for half in range(2):
            rng = slice(half * SUBLANES, (half + 1) * SUBLANES)
            at = pl.ds(pl.multiple_of(i * 2 * SUBLANES + half * SUBLANES, SUBLANES), SUBLANES)
            gates = mixed([t[rng] for t in upg], gtaps_ref, at)
            values = mixed([t[rng] for t in upv], vtaps_ref, at)
            out = []
            for n, (gate, value) in enumerate(zip(gates, values)):
                sigma = jax.nn.sigmoid(gate)
                silu = gate * sigma
                lanes = slice(n * LANES, (n + 1) * LANES)
                silu_ref[at, lanes] = silu
                slope_ref[at, lanes] = value * sigma * (1.0 + gate * (1.0 - sigma))
                out.append(silu * value)
            halves.append(out)
        for n, (top, low) in enumerate(zip(*halves)):
            hidden_ref[both, n * LANES : (n + 1) * LANES] = jnp.concatenate([top, low], axis=0).astype(BF16)
        return carry

    lax.fori_loop(0, height // (2 * SUBLANES), body, 0, unroll=UNROLL)


def forward_part(me, pieces, gate_t, value_t, gtaps, vtaps):
    hidden, model = gate_t.shape
    parts, rows = len(pieces), pieces[0].shape[0]
    tokens, count = parts * rows, gtaps.shape[1]
    height = hidden // CHUNKS
    piece = pl.BlockSpec((rows, model), lambda i, me_ref: (0, 0))
    weight = pl.BlockSpec((height, model), lambda i, me_ref: (i, 0))
    taps = pl.BlockSpec((height, count), lambda i, me_ref: (i, 0))
    out = pl.BlockSpec((height, tokens), lambda i, me_ref: (i, 0))
    return pl.pallas_call(
        functools.partial(forward_kernel, parts),
        out_shape=tuple(jax.ShapeDtypeStruct((hidden, tokens), t) for t in (BF16, F32, F32, BF16, BF16)),
        grid_spec=pltpu.PrefetchScalarGridSpec(
            num_scalar_prefetch=1,
            grid=(CHUNKS,),
            in_specs=[piece] * parts + [weight, weight, taps, taps],
            out_specs=(out,) * 5,
        ),
        compiler_params=pltpu.CompilerParams(dimension_semantics=("arbitrary",), vmem_limit_bytes=LIMIT),
        cost_estimate=pl.CostEstimate(
            flops=4 * hidden * tokens * model, bytes_accessed=18 * hidden * tokens, transcendentals=2 * hidden * tokens
        ),
        name="forward_part",
    )(me, *pieces, gate_t, value_t, gtaps, vtaps)


def backward_kernel(parts, orders, call, me_ref, *refs):
    refs = list(refs)

    def take(count):
        taken, refs[:count] = refs[:count], []
        return taken

    subs = len(orders)
    sources = take(2 * parts + 6)
    gtaps_ref, vtaps_ref = take(2)
    targets = take(2 * subs + 2)
    (sums_ref,) = take(1)
    toks, cots, bufs = take(parts), take(parts), take(6)
    down_ref, hidden_ref, silu_ref, slope_ref, upg_ref, upv_ref = bufs
    outs, (ggrad_ref, vgrad_ref), (back, acc, in_sems, out_sems) = take(2 * subs), take(2), take(4)
    height, rows = down_ref.shape[0], toks[0].shape[0]
    count = gtaps_ref.shape[1]

    here = toks + cots + bufs
    mine = pl.ds(call * height, height)
    arrivals = [
        pltpu.make_async_copy(src if n < 2 * parts else src.at[mine], dst, in_sems.at[n])
        for n, (src, dst) in enumerate(zip(sources, here))
    ]
    order = [2 * parts, *range(parts, 2 * parts), *range(2 * parts + 2, 2 * parts + 6), 2 * parts + 1, *range(parts)]
    for n in order:
        arrivals[n].start()
    leaving = []

    def leave(src, dst):
        copy = pltpu.make_async_copy(src, dst, out_sems.at[len(leaving)])
        copy.start()
        leaving.append(copy)

    spots = [pl.ds(pl.multiple_of((me_ref[0] ^ r) * rows, rows), rows) for r in range(parts)]
    arrivals[2 * parts].wait()
    for r, (at, piece) in enumerate(zip(spots, cots)):
        arrivals[parts + r].wait()
        back[:, at] = dot_rows(down_ref[...], piece[...])
    for n in range(2 * parts + 2, 2 * parts + 6):
        arrivals[n].wait()

    def mixed(tiles, fields, taps_ref, at, first):
        total = None
        for k in range(count):
            tap = jnp.broadcast_to(taps_ref[at, k : k + 1], (SUBLANES, LANES))
            moved = moved_earlier(tiles, k) if k else tiles
            terms = [tap * tile for tile in moved]
            total = terms if total is None else [a + b for a, b in zip(total, terms)]
            acc[first + k, at] = sum(m * f for m, f in zip(moved, fields))
        return total

    def body(i, carry):
        both = pl.ds(pl.multiple_of(i * 2 * SUBLANES, 2 * SUBLANES), 2 * SUBLANES)
        upg = [tile.astype(F32) for tile in load_tiles(upg_ref, both)]
        upv = [tile.astype(F32) for tile in load_tiles(upv_ref, both)]
        gates, values = [], []
        for half in range(2):
            rng = slice(half * SUBLANES, (half + 1) * SUBLANES)
            at = pl.ds(pl.multiple_of(i * 2 * SUBLANES + half * SUBLANES, SUBLANES), SUBLANES)
            up = load_tiles(back, at)
            gback = [a * b for a, b in zip(up, load_tiles(slope_ref, at))]
            gates.append(mixed(gback, [t[rng] for t in upg], gtaps_ref, at, 0))
            vback = [a * b for a, b in zip(up, load_tiles(silu_ref, at))]
            values.append(mixed(vback, [t[rng] for t in upv], vtaps_ref, at, count))
        for ref, halves in ((ggrad_ref, gates), (vgrad_ref, values)):
            for n, (top, low) in enumerate(zip(*halves)):
                ref[both, n * LANES : (n + 1) * LANES] = jnp.concatenate([top, low], axis=0).astype(BF16)
        return carry

    lax.fori_loop(0, height // (2 * SUBLANES), body, 0, unroll=UNROLL)
    leave(ggrad_ref, targets[2 * subs])
    leave(vgrad_ref, targets[2 * subs + 1])
    for n in [2 * parts + 1, *range(parts)]:
        arrivals[n].wait()

    part = height // subs
    size = outs[0].shape[2]
    for pair in (3, 2, 1, 0):
        bits = (pair >> 1, pair & 1)
        cols = pl.ds(pl.multiple_of((me_ref[1] ^ pair) * size, size), size)
        both, down = None, None
        for at, tok, cot in zip(spots, toks, cots):
            term = dot(jnp.concatenate([ggrad_ref[:, at], vgrad_ref[:, at]], axis=0), tok[:, cols])
            both = term if both is None else both + term
            term = dot(hidden_ref[:, at], cot[:, cols])
            down = term if down is None else down + term
        both, down = both.astype(BF16), down.astype(BF16)
        for sub, (first, second) in enumerate(orders):
            which, spot = 2 * sub + 1 - bits[first], bits[second]
            ref, own = outs[which], slice(sub * part, (sub + 1) * part)
            ref[spot, :part] = both[own]
            ref[spot, part : 2 * part] = both[height:][own]
            ref[spot, 2 * part :] = down[own]
            leave(ref.at[spot], targets[which].at[spot])
    for k in range(2 * count):
        sums_ref[:, k : k + 1] = jnp.sum(acc[k], axis=1, keepdims=True)
    for copy in leaving:
        copy.wait()


def backward_part(call, me, toks, cots, down, hidden, silu, slope, upg, upv, gtaps, vtaps):
    full, model = down.shape
    parts, rows = len(toks), toks[0].shape[0]
    tokens, count = parts * rows, gtaps.shape[1]
    height, subs = full // CALLS, CHUNKS // CALLS

    def whole(shape):
        return pl.BlockSpec(shape, lambda i, me_ref: (0,) * len(shape))

    taps = pl.BlockSpec((height, count), lambda i, me_ref: (call, 0))
    payload = (2, 3 * height // subs, model // 4)
    anywhere = pl.BlockSpec(memory_space=pl.ANY)
    shapes = (payload,) * (2 * subs) + ((height, tokens), (height, tokens), (height, 2 * count))
    types = (BF16,) * (2 * subs + 2) + (F32,)
    return pl.pallas_call(
        functools.partial(backward_kernel, parts, ORDERS[call * subs : (call + 1) * subs], call),
        out_shape=tuple(jax.ShapeDtypeStruct(s, t) for s, t in zip(shapes, types)),
        grid_spec=pltpu.PrefetchScalarGridSpec(
            num_scalar_prefetch=1,
            grid=(1,),
            in_specs=[anywhere] * (2 * parts + 6) + [taps, taps],
            out_specs=(anywhere,) * (2 * subs + 2) + (whole(shapes[-1]),),
            scratch_shapes=[
                *[pltpu.VMEM((rows, model), BF16)] * (2 * parts),
                pltpu.VMEM((height, model), BF16),
                *[pltpu.VMEM((height, tokens), t) for t in (BF16, F32, F32, BF16, BF16)],
                *[pltpu.VMEM(payload, BF16)] * (2 * subs),
                *[pltpu.VMEM((height, tokens), BF16)] * 2,
                pltpu.VMEM((height, tokens), F32),
                pltpu.VMEM((2 * count, height, LANES), F32),
                pltpu.SemaphoreType.DMA((2 * parts + 6,)),
                pltpu.SemaphoreType.DMA((4 * subs + 2,)),
            ],
        ),
        compiler_params=pltpu.CompilerParams(dimension_semantics=("arbitrary",), vmem_limit_bytes=LIMIT),
        cost_estimate=pl.CostEstimate(
            flops=8 * height * tokens * model, bytes_accessed=8 * tokens * model, transcendentals=0
        ),
        name="backward_part",
    )(me, *toks, *cots, down, hidden, silu, slope, upg, upv, gtaps, vtaps)


def input_kernel(me_ref, *refs):
    count = (len(refs) - 4) // 2
    ggrads, vgrads = refs[:count], refs[count : 2 * count]
    gate_ref, value_ref, sent_ref, kept_ref = refs[2 * count :]
    height = ggrads[0].shape[0]
    total = None
    for grads, weight_ref in ((ggrads, gate_ref), (vgrads, value_ref)):
        for h, ref in enumerate(grads):
            term = lax.dot_general(
                ref[...], weight_ref[h * height : (h + 1) * height], (((0,), (0,)), ((), ())), preferred_element_type=F32
            )
            total = term if total is None else total + term
    step = pl.program_id(0)

    @pl.when(step < pl.num_programs(0) // 2)
    def _():
        sent_ref[0] = total.astype(BF16)

    @pl.when(step >= pl.num_programs(0) // 2)
    def _():
        kept_ref[0] = total


def input_part(me, ggrads, vgrads, gate_t, value_t, parts):
    hidden, model = gate_t.shape
    height, tokens = ggrads[0].shape
    rows, half = tokens // parts, parts // 2

    def relative(i):
        return jnp.where(i < half, 2 * i + 1, 2 * (i - half))

    field = pl.BlockSpec((height, rows), lambda i, me_ref: (0, me_ref[0] ^ relative(i)))
    weight = pl.BlockSpec((hidden, model), lambda i, me_ref: (0, 0))
    return pl.pallas_call(
        input_kernel,
        out_shape=(
            jax.ShapeDtypeStruct((half, rows, model), BF16),
            jax.ShapeDtypeStruct((half, rows, model), F32),
        ),
        grid_spec=pltpu.PrefetchScalarGridSpec(
            num_scalar_prefetch=1,
            grid=(parts,),
            in_specs=[field] * (2 * len(ggrads)) + [weight, weight],
            out_specs=(
                pl.BlockSpec((1, rows, model), lambda i, me_ref: (jnp.minimum(i, half - 1), 0, 0)),
                pl.BlockSpec((1, rows, model), lambda i, me_ref: (jnp.maximum(i - half, 0), 0, 0)),
            ),
        ),
        compiler_params=pltpu.CompilerParams(dimension_semantics=("arbitrary",), vmem_limit_bytes=LIMIT),
        cost_estimate=pl.CostEstimate(
            flops=4 * hidden * tokens * model, bytes_accessed=4 * hidden * tokens + 6 * tokens * model, transcendentals=0
        ),
        name="input_part",
    )(me, *ggrads, *vgrads, gate_t, value_t)


def add(left, right, dtype):
    return (left.astype(F32) + right.astype(F32)).astype(dtype)


def reduce_chunk(sent, kept, first, second):
    got = exchange(sent, "rep", first)
    over = exchange(add(kept[1], got[1], BF16), "rep", second)
    mine = add(add(kept[0], got[0], F32), over, BF16)
    rest = [b for b in range(bit_count(lax.axis_size("rep"))) if b not in (first, second)]
    for at, bit in enumerate(rest):
        mine = add(mine, exchange(mine, "rep", bit), BF16 if at == len(rest) - 1 else F32)
    pair = jnp.stack([mine, exchange(mine, "rep", second)])
    return pair, exchange(pair, "rep", first)


def place_kernel(scale, where_ref, near_ref, far_ref, *refs):
    outs = refs[-3:]
    height = outs[0].shape[0]
    step = pl.program_id(0)
    for near, ref in ((True, near_ref), (False, far_ref)):

        @pl.when((step < 2) == near)
        def _(ref=ref):
            for n, out_ref in enumerate(outs):
                out_ref[...] = ref[0, n * height : (n + 1) * height].astype(F32) * scale


def place(chunk, where, near, far, outs, shape, scale):
    swap = ORDERS[chunk][0] == 1
    hidden, model = shape
    height, size = hidden // CHUNKS, model // 4
    block = (1, *near.shape[1:])
    first = pl.BlockSpec(block, lambda i, where_ref: (jnp.minimum(i, 1), 0, 0))
    last = pl.BlockSpec(block, lambda i, where_ref: (jnp.maximum(i - 2, 0), 0, 0))

    def spot(i, where_ref):
        return chunk, ((i >> 1) | ((i & 1) << 1) if swap else i) ^ where_ref[1]

    spec = pl.BlockSpec((height, size), spot)
    return pl.pallas_call(
        functools.partial(place_kernel, scale),
        out_shape=(jax.ShapeDtypeStruct(shape, F32),) * 3,
        grid_spec=pltpu.PrefetchScalarGridSpec(
            num_scalar_prefetch=1,
            grid=(4,),
            in_specs=[first, last] + [pl.BlockSpec(memory_space=pl.ANY)] * len(outs),
            out_specs=(spec,) * 3,
        ),
        input_output_aliases={3 + n: n for n in range(len(outs))},
        compiler_params=pltpu.CompilerParams(dimension_semantics=("arbitrary",), vmem_limit_bytes=LIMIT),
        cost_estimate=pl.CostEstimate(flops=3 * height * model, bytes_accessed=18 * height * model, transcendentals=0),
        name="place",
    )(where, near, far, *outs)


def butterfly(value):
    for bit in range(bit_count(lax.axis_size("rep"))):
        value = value + exchange(value, "rep", bit)
    return value


def gather_relative(own):
    found = {0: own}
    base = bit_count(lax.axis_size("tp"))
    for bit in range(bit_count(lax.axis_size("fs"))):
        found.update({r | (1 << (base + bit)): exchange(item, "fs", bit) for r, item in list(found.items())})
    for bit in range(base):
        found.update({r | (1 << bit): exchange(item, "tp", bit) for r, item in list(found.items())})
    return [found[r] for r in range(len(found))]


def scatter_relative(sent, kept):
    moved = exchange(sent, "tp", 0)
    blocks = [add(kept[i], moved[i], F32) for i in range(kept.shape[0])]
    bits = [("tp", b) for b in range(1, bit_count(lax.axis_size("tp")))]
    bits += [("fs", b) for b in range(bit_count(lax.axis_size("fs")))]
    for axis, bit in bits:
        far = jnp.stack(blocks[1::2]).astype(BF16)
        moved = exchange(far, axis, bit)
        blocks = [add(item, moved[i], F32) for i, item in enumerate(blocks[0::2])]
    return blocks[0].astype(BF16)


def layer(tokens, cotangent, gate_weight, value_weight, down_weight, gate_taps, value_taps):
    rows, model = tokens.shape
    hidden = gate_weight.shape[1]
    parts = lax.axis_size("fs") * lax.axis_size("tp")
    scale = 1.0 / math.sqrt(rows * parts * lax.axis_size("rep"))
    me = (lax.axis_index("fs") * lax.axis_size("tp") + lax.axis_index("tp")).astype(jnp.int32)
    gate_t, value_t = gate_weight.T, value_weight.T
    gtaps, vtaps = gate_taps.T, value_taps.T
    where = jnp.stack([me, (2 * rep_bit(0) + rep_bit(1)).astype(jnp.int32)])

    cotangent, where, gtaps, vtaps = lax.optimization_barrier((cotangent, where, gtaps, vtaps))
    toks = gather_relative(tokens)
    cots = gather_relative(cotangent)
    fields = forward_part(where, toks, gate_t, value_t, gtaps, vtaps)
    ggrads, vgrads, sums, done = [], [], [], {}
    subs = CHUNKS // CALLS
    for call in range(CALLS):
        *payload, ggrad, vgrad, tapsum = backward_part(
            call, where, toks, cots, down_weight, *fields, gtaps, vtaps
        )
        for sub in range(subs):
            chunk = call * subs + sub
            done[chunk] = reduce_chunk(payload[2 * sub], payload[2 * sub + 1], *ORDERS[chunk])
        ggrads.append(ggrad)
        vgrads.append(vgrad)
        sums.append(tapsum)
    outs = ()
    for chunk in FINISH:
        outs = place(chunk, where, *done[chunk], outs, (hidden, model), scale)
    sums = butterfly(jnp.concatenate(sums, axis=0).T) * scale
    partial = input_part(where, ggrads, vgrads, gate_t, value_t, parts)
    input_grad = scatter_relative(*partial)
    count = gate_taps.shape[0]
    return input_grad, outs[0].T, outs[1].T, outs[2], sums[:count], sums[count:]


def solution(mesh):
    in_specs = (
        P(("rep", "fs", "tp"), None),
        P(("rep", "fs", "tp"), None),
        P(None, ("fs", "tp")),
        P(None, ("fs", "tp")),
        P(("fs", "tp"), None),
        P(None, ("fs", "tp")),
        P(None, ("fs", "tp")),
    )
    out_specs = (
        P(("rep", "fs", "tp"), None),
        P(None, ("fs", "tp")),
        P(None, ("fs", "tp")),
        P(("fs", "tp"), None),
        P(None, ("fs", "tp")),
        P(None, ("fs", "tp")),
    )
    return jax.shard_map(layer, mesh=mesh, in_specs=in_specs, out_specs=out_specs, check_vma=False)
```

```python
import functools
import math

import jax
import jax.numpy as jnp
from jax import lax
from jax.experimental import pallas as pl
from jax.experimental.pallas import tpu as pltpu
from jax.sharding import PartitionSpec as P


F32 = jnp.float32
BF16 = jnp.bfloat16
LANES = 128
SUBLANES = 8
LIMIT = 60000 * 2**10
BLOCKS = 4
FIRST, SECOND = (0, 1), (1, 0)
GROUPS = (((11, FIRST), (11, SECOND)), ((11, FIRST), (11, SECOND)))
CALLS = ((0,), (1,))


def chunk_rows(hidden):
    total = sum(share for group in GROUPS for share, _ in group)
    assert hidden % total == 0
    unit, start, out = hidden // total, 0, []
    for group in GROUPS:
        heights = [share * unit for share, _ in group]
        out.append((start, sum(heights), heights, [order for _, order in group]))
        start += sum(heights)
    return out


def bit_count(size):
    return size.bit_length() - 1


def exchange(value, axis, bit):
    size = lax.axis_size(axis)
    return lax.ppermute(value, axis, [(i, i ^ (1 << bit)) for i in range(size)])


FINISH = (
    (0, (0, 1)),
    (1, (0, 1)),
    (2, (0,)),
    (3, (0, 1)),
    (2, (1,)),
)


def rep_bit(bit):
    return (lax.axis_index("rep") >> bit) & 1


def dot_rows(left, right):
    return lax.dot_general(left, right, (((1,), (1,)), ((), ())), preferred_element_type=F32)


def dot(left, right):
    return lax.dot_general(left, right, (((1,), (0,)), ((), ())), preferred_element_type=F32)


def lane_index():
    return lax.broadcasted_iota(jnp.int32, (SUBLANES, LANES), 1)


def moved_later(tiles, offset):
    lane = lane_index()
    turned = [pltpu.roll(tile, offset, 1) for tile in tiles]
    before = [jnp.zeros_like(tiles[0])] + turned[:-1]
    return [jnp.where(lane < offset, b, t) for b, t in zip(before, turned)]


def moved_earlier(tiles, offset):
    lane = lane_index()
    turned = [pltpu.roll(tile, LANES - offset, 1) for tile in tiles]
    after = turned[1:] + [jnp.zeros_like(tiles[0])]
    return [jnp.where(lane >= LANES - offset, a, t) for a, t in zip(after, turned)]


def load_tiles(ref, at):
    return [ref[at, i : i + LANES] for i in range(0, ref.shape[1], LANES)]


def forward_kernel(parts, me_ref, *refs):
    pieces = refs[:parts]
    gate_ref, value_ref, gtaps_ref, vtaps_ref = refs[parts : parts + 4]
    hidden_ref, silu_ref, slope_ref, upg_ref, upv_ref = refs[parts + 4 :]
    height = gate_ref.shape[0]
    rows = pieces[0].shape[0]
    count = gtaps_ref.shape[1]
    weights = jnp.concatenate([gate_ref[...], value_ref[...]], axis=0)
    for r, piece in enumerate(pieces):
        at = pl.ds(pl.multiple_of((me_ref[0] ^ r) * rows, rows), rows)
        up = dot_rows(weights, piece[...]).astype(BF16)
        upg_ref[:, at] = up[:height]
        upv_ref[:, at] = up[height:]

    def mixed(tiles, taps_ref, at):
        total = None
        for k in range(count):
            tap = jnp.broadcast_to(taps_ref[at, k : k + 1], (SUBLANES, LANES))
            terms = [tap * tile for tile in (moved_later(tiles, k) if k else tiles)]
            total = terms if total is None else [a + b for a, b in zip(total, terms)]
        return total

    def body(i, carry):
        both = pl.ds(pl.multiple_of(i * 2 * SUBLANES, 2 * SUBLANES), 2 * SUBLANES)
        upg = [tile.astype(F32) for tile in load_tiles(upg_ref, both)]
        upv = [tile.astype(F32) for tile in load_tiles(upv_ref, both)]
        halves = []
        for half in range(2):
            rng = slice(half * SUBLANES, (half + 1) * SUBLANES)
            at = pl.ds(pl.multiple_of(i * 2 * SUBLANES + half * SUBLANES, SUBLANES), SUBLANES)
            gates = mixed([t[rng] for t in upg], gtaps_ref, at)
            values = mixed([t[rng] for t in upv], vtaps_ref, at)
            out = []
            for gate, value in zip(gates, values):
                sigma = jax.nn.sigmoid(gate)
                silu = gate * sigma
                out.append((silu * value, silu, value * sigma * (1.0 + gate * (1.0 - sigma))))
            halves.append(out)
        for n, (tops, lows) in enumerate(zip(*halves)):
            for ref, top, low in zip((hidden_ref, silu_ref, slope_ref), tops, lows):
                ref[both, n * LANES : (n + 1) * LANES] = jnp.concatenate([top, low], axis=0).astype(ref.dtype)
        return carry

    lax.fori_loop(0, height // (2 * SUBLANES), body, 0)


def forward_part(me, pieces, gate_t, value_t, gtaps, vtaps):
    hidden, model = gate_t.shape
    parts, rows = len(pieces), pieces[0].shape[0]
    tokens, count = parts * rows, gtaps.shape[1]
    height = hidden // BLOCKS
    piece = pl.BlockSpec((rows, model), lambda i, me_ref: (0, 0))
    weight = pl.BlockSpec((height, model), lambda i, me_ref: (i, 0))
    taps = pl.BlockSpec((height, count), lambda i, me_ref: (i, 0))
    out = pl.BlockSpec((height, tokens), lambda i, me_ref: (i, 0))
    return pl.pallas_call(
        functools.partial(forward_kernel, parts),
        out_shape=tuple(jax.ShapeDtypeStruct((hidden, tokens), t) for t in (BF16, F32, F32, BF16, BF16)),
        grid_spec=pltpu.PrefetchScalarGridSpec(
            num_scalar_prefetch=1,
            grid=(BLOCKS,),
            in_specs=[piece] * parts + [weight, weight, taps, taps],
            out_specs=(out,) * 5,
        ),
        compiler_params=pltpu.CompilerParams(dimension_semantics=("arbitrary",), vmem_limit_bytes=LIMIT),
        cost_estimate=pl.CostEstimate(
            flops=4 * hidden * tokens * model, bytes_accessed=18 * hidden * tokens, transcendentals=2 * hidden * tokens
        ),
        name="forward_part",
    )(me, *pieces, gate_t, value_t, gtaps, vtaps)


def backward_kernel(parts, groups, me_ref, *refs):
    refs = list(refs)

    def take(count):
        taken, refs[:count] = refs[:count], []
        return taken

    outs_count = sum(2 * len(group[2]) for group in groups)
    sources = take(2 * parts + 6)
    gtaps_ref, vtaps_ref = take(2)
    targets = take(outs_count + 2)
    all_sums = take(len(groups))
    toks, cots, bufs = take(parts), take(parts), take(6)
    outs, grads, (back, acc, in_sems, out_sems) = take(outs_count), take(2), take(4)
    rows = toks[0].shape[0]
    count = gtaps_ref.shape[1]
    offset = groups[0][0]

    started, arrivals, leaving = {}, {}, []
    for n, (src, dst) in enumerate(zip(sources[: 2 * parts], toks + cots)):
        arrivals[n] = (src, dst)
    for g, (start, height, _, _) in enumerate(groups):
        for n, (src, dst) in enumerate(zip(sources[2 * parts :], bufs)):
            arrivals[g, n] = (src.at[pl.ds(start, height)], dst.at[pl.ds(start - offset, height)])

    def begin(*keys):
        for key in keys:
            src, dst = arrivals[key]
            started[key] = pltpu.make_async_copy(src, dst, in_sems.at[len(started)])
            started[key].start()

    def arrived(*keys):
        for key in keys:
            started[key].wait()

    def leave(src, dst):
        copy = pltpu.make_async_copy(src, dst, out_sems.at[len(leaving)])
        copy.start()
        leaving.append(copy)

    spots = [pl.ds(pl.multiple_of((me_ref[0] ^ r) * rows, rows), rows) for r in range(parts)]
    fields = (2, 3, 4, 5)
    begin((0, 0), *range(parts, 2 * parts), *[(0, n) for n in fields])
    base_out = 0
    for g, (start, height, heights, orders) in enumerate(groups):
        low = start - offset
        down_ref, hidden_ref, silu_ref, slope_ref, upg_ref, upv_ref = [buf.at[low : low + height] for buf in bufs]
        ggrad_ref, vgrad_ref = [grad.at[low : low + height] for grad in grads]
        gtaps, vtaps = gtaps_ref.at[low : low + height], vtaps_ref.at[low : low + height]
        arrived((g, 0))
        for r, (at, piece) in enumerate(zip(spots, cots)):
            if g == 0:
                arrived(parts + r)
            back[:height, at] = dot_rows(down_ref[...], piece[...])
        begin((g, 1), *(range(parts) if g == 0 else ()))
        if g + 1 < len(groups):
            begin((g + 1, 0), *[(g + 1, n) for n in fields])
        arrived(*[(g, n) for n in fields])

        def mixed(tiles, fields, taps_ref, at, first):
            total = None
            for k in range(count):
                tap = jnp.broadcast_to(taps_ref[at, k : k + 1], (SUBLANES, LANES))
                moved = moved_earlier(tiles, k) if k else tiles
                terms = [tap * tile for tile in moved]
                total = terms if total is None else [a + b for a, b in zip(total, terms)]
                acc[first + k, at] = sum(m * f for m, f in zip(moved, fields))
            return total

        def body(i, carry):
            both = pl.ds(pl.multiple_of(i * 2 * SUBLANES, 2 * SUBLANES), 2 * SUBLANES)
            upg = [tile.astype(F32) for tile in load_tiles(upg_ref, both)]
            upv = [tile.astype(F32) for tile in load_tiles(upv_ref, both)]
            gates, values = [], []
            for half in range(2):
                rng = slice(half * SUBLANES, (half + 1) * SUBLANES)
                at = pl.ds(pl.multiple_of(i * 2 * SUBLANES + half * SUBLANES, SUBLANES), SUBLANES)
                up = load_tiles(back, at)
                gback = [a * b for a, b in zip(up, load_tiles(slope_ref, at))]
                gates.append(mixed(gback, [t[rng] for t in upg], gtaps, at, 0))
                vback = [a * b for a, b in zip(up, load_tiles(silu_ref, at))]
                values.append(mixed(vback, [t[rng] for t in upv], vtaps, at, count))
            for ref, halves in ((ggrad_ref, gates), (vgrad_ref, values)):
                for n, (top, bottom) in enumerate(zip(*halves)):
                    ref[both, n * LANES : (n + 1) * LANES] = jnp.concatenate([top, bottom], axis=0).astype(BF16)
            return carry

        lax.fori_loop(0, height // (2 * SUBLANES), body, 0)
        leave(ggrad_ref, targets[outs_count].at[low : low + height])
        leave(vgrad_ref, targets[outs_count + 1].at[low : low + height])
        arrived((g, 1), *(range(parts) if g == 0 else ()))

        size = outs[0].shape[2]
        for pair in (3, 2, 1, 0):
            bits = (pair >> 1, pair & 1)
            cols = pl.ds(pl.multiple_of((me_ref[1] ^ pair) * size, size), size)
            both, down = None, None
            for at, tok, cot in zip(spots, toks, cots):
                term = dot(jnp.concatenate([ggrad_ref[:, at], vgrad_ref[:, at]], axis=0), tok[:, cols])
                both = term if both is None else both + term
                term = dot(hidden_ref[:, at], cot[:, cols])
                down = term if down is None else down + term
            both, down = both.astype(BF16), down.astype(BF16)
            top = 0
            for sub, (part, (first, second)) in enumerate(zip(heights, orders)):
                which, spot = base_out + 2 * sub + 1 - bits[first], bits[second]
                ref, own = outs[which], slice(top, top + part)
                ref[spot, :part] = both[own]
                ref[spot, part : 2 * part] = both[height:][own]
                ref[spot, 2 * part :] = down[own]
                leave(ref.at[spot], targets[which].at[spot])
                top += part
        ones = jnp.ones((SUBLANES, LANES), F32)
        for k in range(2 * count):
            total = lax.dot_general(
                ones, acc[k, :height], (((1,), (1,)), ((), ())), precision=lax.Precision.HIGHEST, preferred_element_type=F32
            )
            all_sums[g][k : k + 1] = total[:1]
        base_out += 2 * len(heights)
    for copy in leaving:
        copy.wait()


def backward_part(groups, me, toks, cots, down, hidden, silu, slope, upg, upv, gtaps, vtaps):
    model = down.shape[1]
    parts, rows = len(toks), toks[0].shape[0]
    tokens, count = parts * rows, gtaps.shape[1]
    height, most = sum(group[1] for group in groups), max(group[1] for group in groups)
    offset = groups[0][0]
    payloads = [(2, 3 * part, model // 4) for group in groups for part in group[2] for _ in range(2)]
    anywhere = pl.BlockSpec(memory_space=pl.ANY)
    vmem = pl.BlockSpec(memory_space=pltpu.VMEM)
    sums = [(2 * count, group[1]) for group in groups]
    shapes = (*payloads, (height, tokens), (height, tokens), *sums)
    types = (BF16,) * (len(payloads) + 2) + (F32,) * len(sums)
    mine = slice(offset, offset + height)
    return pl.pallas_call(
        functools.partial(backward_kernel, parts, groups),
        out_shape=tuple(jax.ShapeDtypeStruct(s, t) for s, t in zip(shapes, types)),
        grid_spec=pltpu.PrefetchScalarGridSpec(
            num_scalar_prefetch=1,
            grid=(1,),
            in_specs=[anywhere] * (2 * parts + 6) + [vmem, vmem],
            out_specs=(anywhere,) * (len(payloads) + 2) + (vmem,) * len(sums),
            scratch_shapes=[
                *[pltpu.VMEM((rows, model), BF16)] * (2 * parts),
                pltpu.VMEM((height, model), BF16),
                *[pltpu.VMEM((height, tokens), t) for t in (BF16, F32, F32, BF16, BF16)],
                *[pltpu.VMEM(shape, BF16) for shape in payloads],
                *[pltpu.VMEM((height, tokens), BF16)] * 2,
                pltpu.VMEM((most, tokens), F32),
                pltpu.VMEM((2 * count, most, LANES), F32),
                pltpu.SemaphoreType.DMA((2 * parts + 6 * len(groups),)),
                pltpu.SemaphoreType.DMA((2 * len(payloads) + 2 * len(groups),)),
            ],
        ),
        compiler_params=pltpu.CompilerParams(dimension_semantics=("arbitrary",), vmem_limit_bytes=LIMIT),
        cost_estimate=pl.CostEstimate(
            flops=8 * height * tokens * model, bytes_accessed=8 * tokens * model, transcendentals=0
        ),
        name="backward_part",
    )(me, *toks, *cots, down, hidden, silu, slope, upg, upv, gtaps[mine], vtaps[mine])


def input_kernel(me_ref, *refs):
    count = (len(refs) - 3) // 2
    ggrads, vgrads = refs[:count], refs[count : 2 * count]
    gate_ref, value_ref, out_ref = refs[2 * count :]
    total = None
    for grads, weight_ref in ((ggrads, gate_ref), (vgrads, value_ref)):
        low = 0
        for ref in grads:
            high = low + ref.shape[0]
            term = lax.dot_general(
                ref[...], weight_ref[low:high], (((0,), (0,)), ((), ())), preferred_element_type=F32
            )
            total = term if total is None else total + term
            low = high
    out_ref[0] = total.astype(out_ref.dtype)


def input_part(me, ggrads, vgrads, gate_t, value_t, parts, odd, dtype):
    hidden, model = gate_t.shape
    tokens = ggrads[0].shape[1]
    rows, half = tokens // parts, parts // 2
    fields = [pl.BlockSpec((g.shape[0], rows), lambda i, me_ref: (0, me_ref[0] ^ (2 * i + odd))) for g in ggrads]
    weight = pl.BlockSpec((hidden, model), lambda i, me_ref: (0, 0))
    return pl.pallas_call(
        input_kernel,
        out_shape=jax.ShapeDtypeStruct((half, rows, model), dtype),
        grid_spec=pltpu.PrefetchScalarGridSpec(
            num_scalar_prefetch=1,
            grid=(half,),
            in_specs=fields * 2 + [weight, weight],
            out_specs=pl.BlockSpec((1, rows, model), lambda i, me_ref: (i, 0, 0)),
        ),
        compiler_params=pltpu.CompilerParams(dimension_semantics=("arbitrary",), vmem_limit_bytes=LIMIT),
        cost_estimate=pl.CostEstimate(
            flops=2 * hidden * tokens * model, bytes_accessed=2 * hidden * tokens + 3 * tokens * model, transcendentals=0
        ),
        name="input_part",
    )(me, *ggrads, *vgrads, gate_t, value_t)


def add(left, right, dtype):
    return (left.astype(F32) + right.astype(F32)).astype(dtype)


def reduce_chunk(sent, kept, first, second):
    got = exchange(sent, "rep", first)
    half = add(kept[1], got[1], BF16)
    over = exchange(half, "rep", second)
    mine = add(add(kept[0], got[0], F32), over, BF16)
    rest = [b for b in range(bit_count(lax.axis_size("rep"))) if b not in (first, second)]
    for at, bit in enumerate(rest):
        theirs = exchange(mine, "rep", bit)
        mine = add(mine, theirs, BF16 if at == len(rest) - 1 else F32)
    other = exchange(mine, "rep", second)
    pair = jnp.stack([mine, other])
    return pair, exchange(pair, "rep", first)


def place_kernel(scale, start, sides, swap, count, where_ref, *refs):
    pairs, refs = refs[: len(sides)], refs[len(sides) :]
    outs, (stage, out_sems) = refs[count : count + 3], refs[count + 3 :]
    height, size = stage.shape[2:]
    leaving = []
    for i, (pair, spot) in enumerate((pair.at[i], 2 * side + i) for pair, side in zip(pairs, sides) for i in range(2)):
        spot = ((spot >> 1) | ((spot & 1) << 1) if swap else spot) ^ where_ref[1]
        cols = pl.ds(pl.multiple_of(spot * size, size), size)
        for n, out_ref in enumerate(outs):
            stage[i, n] = pair[n * height : (n + 1) * height].astype(F32) * scale
            copy = pltpu.make_async_copy(stage.at[i, n], out_ref.at[pl.ds(start, height), cols], out_sems.at[i, n])
            copy.start()
            leaving.append(copy)
    for copy in leaving:
        copy.wait()


def place(start, height, sides, swap, where, pairs, outs, shape, scale):
    model = shape[1]
    anywhere = pl.BlockSpec(memory_space=pl.ANY)
    blocks = 2 * len(sides)
    return pl.pallas_call(
        functools.partial(place_kernel, scale, start, sides, swap, len(outs)),
        out_shape=(jax.ShapeDtypeStruct(shape, F32),) * 3,
        grid_spec=pltpu.PrefetchScalarGridSpec(
            num_scalar_prefetch=1,
            grid=(1,),
            in_specs=[pl.BlockSpec(memory_space=pltpu.VMEM)] * len(pairs) + [anywhere] * len(outs),
            out_specs=(anywhere,) * 3,
            scratch_shapes=[
                pltpu.VMEM((blocks, 3, height, model // 4), F32),
                pltpu.SemaphoreType.DMA((blocks, 3)),
            ],
        ),
        input_output_aliases={1 + len(pairs) + n: n for n in range(len(outs))},
        compiler_params=pltpu.CompilerParams(dimension_semantics=("arbitrary",), vmem_limit_bytes=LIMIT // 4),
        cost_estimate=pl.CostEstimate(
            flops=3 * height * model, bytes_accessed=9 * blocks // 2 * height * model, transcendentals=0
        ),
        name="place",
    )(where, *pairs, *outs)


def butterfly(value):
    for bit in range(bit_count(lax.axis_size("rep"))):
        value = value + exchange(value, "rep", bit)
    return value


def gather_relative(own):
    found = {0: own}
    base = bit_count(lax.axis_size("tp"))
    for bit in range(bit_count(lax.axis_size("fs"))):
        found.update({r | (1 << (base + bit)): exchange(item, "fs", bit) for r, item in list(found.items())})
    for bit in range(base):
        found.update({r | (1 << bit): exchange(item, "tp", bit) for r, item in list(found.items())})
    return [found[r] for r in range(len(found))]


def scatter_relative(sent, kept):
    moved = exchange(sent, "tp", 0)
    blocks = [add(kept[i], moved[i], F32) for i in range(kept.shape[0])]
    bits = [("tp", b) for b in range(1, bit_count(lax.axis_size("tp")))]
    bits += [("fs", b) for b in range(bit_count(lax.axis_size("fs")))]
    for axis, bit in bits:
        far = jnp.stack(blocks[1::2]).astype(BF16)
        moved = exchange(far, axis, bit)
        blocks = [add(item, moved[i], F32) for i, item in enumerate(blocks[0::2])]
    return blocks[0].astype(BF16)


def layer(tokens, cotangent, gate_weight, value_weight, down_weight, gate_taps, value_taps):
    rows, model = tokens.shape
    hidden = gate_weight.shape[1]
    parts = lax.axis_size("fs") * lax.axis_size("tp")
    scale = 1.0 / math.sqrt(rows * parts * lax.axis_size("rep"))
    me = (lax.axis_index("fs") * lax.axis_size("tp") + lax.axis_index("tp")).astype(jnp.int32)
    gate_t, value_t = gate_weight.T, value_weight.T
    gtaps, vtaps = gate_taps.T, value_taps.T
    where = jnp.stack([me, (2 * rep_bit(0) + rep_bit(1)).astype(jnp.int32)])

    cotangent, where, gtaps, vtaps = lax.optimization_barrier((cotangent, where, gtaps, vtaps))
    toks = gather_relative(tokens)
    cots = gather_relative(cotangent)
    fields = forward_part(where, toks, gate_t, value_t, gtaps, vtaps)
    ggrads, vgrads, sums, chunks = [], [], [], []
    groups = chunk_rows(hidden)
    for members in CALLS:
        mine = [groups[g] for g in members]
        found = backward_part(mine, where, toks, cots, down_weight, *fields, gtaps, vtaps)
        *payload, ggrad, vgrad = found[: len(found) - len(mine)]
        sums.extend(found[len(found) - len(mine) :])
        for start, _, heights, orders in mine:
            for height, order in zip(heights, orders):
                sent, kept, *payload = payload
                pairs = reduce_chunk(sent, kept, *order)
                chunks.append((start, height, order[0] == 1, pairs))
                start += height
        ggrads.append(ggrad)
        vgrads.append(vgrad)
    outs = ()
    for chunk, sides in FINISH:
        start, height, swap, pairs = chunks[chunk]
        picked = [pairs[side] for side in sides]
        outs = place(start, height, sides, swap, where, picked, outs, (hidden, model), scale)
    sums = butterfly(jnp.concatenate(sums, axis=1)) * scale
    away = input_part(where, ggrads, vgrads, gate_t, value_t, parts, 1, BF16)
    own = input_part(where, ggrads, vgrads, gate_t, value_t, parts, 0, F32)
    input_grad = scatter_relative(away, own)
    count = gate_taps.shape[0]
    return input_grad, outs[0].T, outs[1].T, outs[2], sums[:count], sums[count:]


def solution(mesh):
    in_specs = (
        P(("rep", "fs", "tp"), None),
        P(("rep", "fs", "tp"), None),
        P(None, ("fs", "tp")),
        P(None, ("fs", "tp")),
        P(("fs", "tp"), None),
        P(None, ("fs", "tp")),
        P(None, ("fs", "tp")),
    )
    out_specs = (
        P(("rep", "fs", "tp"), None),
        P(None, ("fs", "tp")),
        P(None, ("fs", "tp")),
        P(("fs", "tp"), None),
        P(None, ("fs", "tp")),
        P(None, ("fs", "tp")),
    )
    return jax.shard_map(layer, mesh=mesh, in_specs=in_specs, out_specs=out_specs, check_vma=False)
```

```python
import functools
import math

import jax
import jax.numpy as jnp
from jax import lax
from jax.experimental import pallas as pl
from jax.experimental.pallas import tpu as pltpu
from jax.sharding import PartitionSpec as P


F32 = jnp.float32
BF16 = jnp.bfloat16
LANES = 128
SUBLANES = 8
LIMIT = 60000 * 2**10
BLOCKS = 4
FIRST, SECOND = (0, 1), (1, 0)
GROUPS = (((11, FIRST), (11, SECOND)), ((11, FIRST), (11, SECOND)))
CALLS = ((0,), (1,))


def chunk_rows(hidden):
    total = sum(share for group in GROUPS for share, _ in group)
    assert hidden % total == 0
    unit, start, out = hidden // total, 0, []
    for group in GROUPS:
        heights = [share * unit for share, _ in group]
        out.append((start, sum(heights), heights, [order for _, order in group]))
        start += sum(heights)
    return out


def bit_count(size):
    return size.bit_length() - 1


def exchange(value, axis, bit):
    size = lax.axis_size(axis)
    return lax.ppermute(value, axis, [(i, i ^ (1 << bit)) for i in range(size)])


FINISH = (
    (0, (0, 1)),
    (1, (0, 1)),
    (2, (0,)),
    (2, (1,)),
    (3, (0, 1)),
)


def rep_bit(bit):
    return (lax.axis_index("rep") >> bit) & 1


def dot_rows(left, right):
    return lax.dot_general(left, right, (((1,), (1,)), ((), ())), preferred_element_type=F32)


def dot(left, right):
    return lax.dot_general(left, right, (((1,), (0,)), ((), ())), preferred_element_type=F32)


def lane_index():
    return lax.broadcasted_iota(jnp.int32, (SUBLANES, LANES), 1)


def moved_later(tiles, offset):
    lane = lane_index()
    turned = [pltpu.roll(tile, offset, 1) for tile in tiles]
    before = [jnp.zeros_like(tiles[0])] + turned[:-1]
    return [jnp.where(lane < offset, b, t) for b, t in zip(before, turned)]


def moved_earlier(tiles, offset):
    lane = lane_index()
    turned = [pltpu.roll(tile, LANES - offset, 1) for tile in tiles]
    after = turned[1:] + [jnp.zeros_like(tiles[0])]
    return [jnp.where(lane >= LANES - offset, a, t) for a, t in zip(after, turned)]


def load_tiles(ref, at):
    return [ref[at, i : i + LANES] for i in range(0, ref.shape[1], LANES)]


def forward_kernel(parts, me_ref, *refs):
    pieces = refs[:parts]
    gate_ref, value_ref, gtaps_ref, vtaps_ref = refs[parts : parts + 4]
    hidden_ref, silu_ref, slope_ref, upg_ref, upv_ref = refs[parts + 4 :]
    height = gate_ref.shape[0]
    rows = pieces[0].shape[0]
    count = gtaps_ref.shape[1]
    weights = jnp.concatenate([gate_ref[...], value_ref[...]], axis=0)
    for r, piece in enumerate(pieces):
        at = pl.ds(pl.multiple_of((me_ref[0] ^ r) * rows, rows), rows)
        up = dot_rows(weights, piece[...]).astype(BF16)
        upg_ref[:, at] = up[:height]
        upv_ref[:, at] = up[height:]

    def mixed(tiles, taps_ref, at):
        total = None
        for k in range(count):
            tap = jnp.broadcast_to(taps_ref[at, k : k + 1], (SUBLANES, LANES))
            terms = [tap * tile for tile in (moved_later(tiles, k) if k else tiles)]
            total = terms if total is None else [a + b for a, b in zip(total, terms)]
        return total

    def body(i, carry):
        both = pl.ds(pl.multiple_of(i * 2 * SUBLANES, 2 * SUBLANES), 2 * SUBLANES)
        upg = [tile.astype(F32) for tile in load_tiles(upg_ref, both)]
        upv = [tile.astype(F32) for tile in load_tiles(upv_ref, both)]
        halves = []
        for half in range(2):
            rng = slice(half * SUBLANES, (half + 1) * SUBLANES)
            at = pl.ds(pl.multiple_of(i * 2 * SUBLANES + half * SUBLANES, SUBLANES), SUBLANES)
            gates = mixed([t[rng] for t in upg], gtaps_ref, at)
            values = mixed([t[rng] for t in upv], vtaps_ref, at)
            out = []
            for gate, value in zip(gates, values):
                sigma = jax.nn.sigmoid(gate)
                silu = gate * sigma
                out.append((silu * value, silu, value * sigma * (1.0 + gate * (1.0 - sigma))))
            halves.append(out)
        for n, (tops, lows) in enumerate(zip(*halves)):
            for ref, top, low in zip((hidden_ref, silu_ref, slope_ref), tops, lows):
                ref[both, n * LANES : (n + 1) * LANES] = jnp.concatenate([top, low], axis=0).astype(ref.dtype)
        return carry

    lax.fori_loop(0, height // (2 * SUBLANES), body, 0)


def forward_part(me, pieces, gate_t, value_t, gtaps, vtaps):
    hidden, model = gate_t.shape
    parts, rows = len(pieces), pieces[0].shape[0]
    tokens, count = parts * rows, gtaps.shape[1]
    height = hidden // BLOCKS
    piece = pl.BlockSpec((rows, model), lambda i, me_ref: (0, 0))
    weight = pl.BlockSpec((height, model), lambda i, me_ref: (i, 0))
    taps = pl.BlockSpec((height, count), lambda i, me_ref: (i, 0))
    out = pl.BlockSpec((height, tokens), lambda i, me_ref: (i, 0))
    return pl.pallas_call(
        functools.partial(forward_kernel, parts),
        out_shape=tuple(jax.ShapeDtypeStruct((hidden, tokens), t) for t in (BF16, F32, F32, BF16, BF16)),
        grid_spec=pltpu.PrefetchScalarGridSpec(
            num_scalar_prefetch=1,
            grid=(BLOCKS,),
            in_specs=[piece] * parts + [weight, weight, taps, taps],
            out_specs=(out,) * 5,
        ),
        compiler_params=pltpu.CompilerParams(dimension_semantics=("arbitrary",), vmem_limit_bytes=LIMIT),
        cost_estimate=pl.CostEstimate(
            flops=4 * hidden * tokens * model, bytes_accessed=18 * hidden * tokens, transcendentals=2 * hidden * tokens
        ),
        name="forward_part",
    )(me, *pieces, gate_t, value_t, gtaps, vtaps)


def backward_kernel(parts, groups, me_ref, *refs):
    refs = list(refs)

    def take(count):
        taken, refs[:count] = refs[:count], []
        return taken

    outs_count = sum(2 * len(group[2]) for group in groups)
    sources = take(2 * parts + 6)
    gtaps_ref, vtaps_ref = take(2)
    targets = take(outs_count + 2)
    all_sums = take(len(groups))
    toks, cots, bufs = take(parts), take(parts), take(6)
    outs, grads, (back, acc, in_sems, out_sems) = take(outs_count), take(2), take(4)
    rows = toks[0].shape[0]
    count = gtaps_ref.shape[1]
    offset = groups[0][0]

    started, arrivals, leaving = {}, {}, []
    for n, (src, dst) in enumerate(zip(sources[: 2 * parts], toks + cots)):
        arrivals[n] = (src, dst)
    for g, (start, height, _, _) in enumerate(groups):
        for n, (src, dst) in enumerate(zip(sources[2 * parts :], bufs)):
            arrivals[g, n] = (src.at[pl.ds(start, height)], dst.at[pl.ds(start - offset, height)])

    def begin(*keys):
        for key in keys:
            src, dst = arrivals[key]
            started[key] = pltpu.make_async_copy(src, dst, in_sems.at[len(started)])
            started[key].start()

    def arrived(*keys):
        for key in keys:
            started[key].wait()

    def leave(src, dst):
        copy = pltpu.make_async_copy(src, dst, out_sems.at[len(leaving)])
        copy.start()
        leaving.append(copy)

    spots = [pl.ds(pl.multiple_of((me_ref[0] ^ r) * rows, rows), rows) for r in range(parts)]
    fields = (2, 3, 4, 5)
    begin((0, 0), *range(parts, 2 * parts), *[(0, n) for n in fields])
    base_out = 0
    for g, (start, height, heights, orders) in enumerate(groups):
        low = start - offset
        down_ref, hidden_ref, silu_ref, slope_ref, upg_ref, upv_ref = [buf.at[low : low + height] for buf in bufs]
        ggrad_ref, vgrad_ref = [grad.at[low : low + height] for grad in grads]
        gtaps, vtaps = gtaps_ref.at[start : start + height], vtaps_ref.at[start : start + height]
        arrived((g, 0))
        for r, (at, piece) in enumerate(zip(spots, cots)):
            if g == 0:
                arrived(parts + r)
            back[:height, at] = dot_rows(down_ref[...], piece[...])
        begin((g, 1), *(range(parts) if g == 0 else ()))
        if g + 1 < len(groups):
            begin((g + 1, 0), *[(g + 1, n) for n in fields])
        arrived(*[(g, n) for n in fields])

        def mixed(tiles, fields, taps_ref, at, first):
            total = None
            for k in range(count):
                tap = jnp.broadcast_to(taps_ref[at, k : k + 1], (SUBLANES, LANES))
                moved = moved_earlier(tiles, k) if k else tiles
                terms = [tap * tile for tile in moved]
                total = terms if total is None else [a + b for a, b in zip(total, terms)]
                acc[first + k, at] = sum(m * f for m, f in zip(moved, fields))
            return total

        def body(i, carry):
            both = pl.ds(pl.multiple_of(i * 2 * SUBLANES, 2 * SUBLANES), 2 * SUBLANES)
            upg = [tile.astype(F32) for tile in load_tiles(upg_ref, both)]
            upv = [tile.astype(F32) for tile in load_tiles(upv_ref, both)]
            gates, values = [], []
            for half in range(2):
                rng = slice(half * SUBLANES, (half + 1) * SUBLANES)
                at = pl.ds(pl.multiple_of(i * 2 * SUBLANES + half * SUBLANES, SUBLANES), SUBLANES)
                up = load_tiles(back, at)
                gback = [a * b for a, b in zip(up, load_tiles(slope_ref, at))]
                gates.append(mixed(gback, [t[rng] for t in upg], gtaps, at, 0))
                vback = [a * b for a, b in zip(up, load_tiles(silu_ref, at))]
                values.append(mixed(vback, [t[rng] for t in upv], vtaps, at, count))
            for ref, halves in ((ggrad_ref, gates), (vgrad_ref, values)):
                for n, (top, bottom) in enumerate(zip(*halves)):
                    ref[both, n * LANES : (n + 1) * LANES] = jnp.concatenate([top, bottom], axis=0).astype(BF16)
            return carry

        lax.fori_loop(0, height // (2 * SUBLANES), body, 0)
        leave(ggrad_ref, targets[outs_count].at[low : low + height])
        leave(vgrad_ref, targets[outs_count + 1].at[low : low + height])
        arrived((g, 1), *(range(parts) if g == 0 else ()))

        size = outs[0].shape[2]
        for pair in (3, 2, 1, 0):
            bits = (pair >> 1, pair & 1)
            cols = pl.ds(pl.multiple_of((me_ref[1] ^ pair) * size, size), size)
            both, down = None, None
            for at, tok, cot in zip(spots, toks, cots):
                term = dot(jnp.concatenate([ggrad_ref[:, at], vgrad_ref[:, at]], axis=0), tok[:, cols])
                both = term if both is None else both + term
                term = dot(hidden_ref[:, at], cot[:, cols])
                down = term if down is None else down + term
            both, down = both.astype(BF16), down.astype(BF16)
            top = 0
            for sub, (part, (first, second)) in enumerate(zip(heights, orders)):
                which, spot = base_out + 2 * sub + 1 - bits[first], bits[second]
                ref, own = outs[which], slice(top, top + part)
                ref[spot, :part] = both[own]
                ref[spot, part : 2 * part] = both[height:][own]
                ref[spot, 2 * part :] = down[own]
                leave(ref.at[spot], targets[which].at[spot])
                top += part
        ones = jnp.ones((SUBLANES, LANES), F32)
        for k in range(2 * count):
            total = lax.dot_general(
                ones, acc[k, :height], (((1,), (1,)), ((), ())), precision=lax.Precision.HIGHEST, preferred_element_type=F32
            )
            all_sums[g][k : k + 1] = total[:1]
        base_out += 2 * len(heights)
    for copy in leaving:
        copy.wait()


def backward_part(groups, me, toks, cots, down, hidden, silu, slope, upg, upv, gtaps, vtaps):
    model = down.shape[1]
    parts, rows = len(toks), toks[0].shape[0]
    tokens, count = parts * rows, gtaps.shape[1]
    height, most = sum(group[1] for group in groups), max(group[1] for group in groups)
    payloads = [(2, 3 * part, model // 4) for group in groups for part in group[2] for _ in range(2)]
    anywhere = pl.BlockSpec(memory_space=pl.ANY)
    vmem = pl.BlockSpec(memory_space=pltpu.VMEM)
    sums = [(2 * count, group[1]) for group in groups]
    shapes = (*payloads, (height, tokens), (height, tokens), *sums)
    types = (BF16,) * (len(payloads) + 2) + (F32,) * len(sums)
    return pl.pallas_call(
        functools.partial(backward_kernel, parts, groups),
        out_shape=tuple(jax.ShapeDtypeStruct(s, t) for s, t in zip(shapes, types)),
        grid_spec=pltpu.PrefetchScalarGridSpec(
            num_scalar_prefetch=1,
            grid=(1,),
            in_specs=[anywhere] * (2 * parts + 6) + [vmem, vmem],
            out_specs=(anywhere,) * (len(payloads) + 2) + (vmem,) * len(sums),
            scratch_shapes=[
                *[pltpu.VMEM((rows, model), BF16)] * (2 * parts),
                pltpu.VMEM((height, model), BF16),
                *[pltpu.VMEM((height, tokens), t) for t in (BF16, F32, F32, BF16, BF16)],
                *[pltpu.VMEM(shape, BF16) for shape in payloads],
                *[pltpu.VMEM((height, tokens), BF16)] * 2,
                pltpu.VMEM((most, tokens), F32),
                pltpu.VMEM((2 * count, most, LANES), F32),
                pltpu.SemaphoreType.DMA((2 * parts + 6 * len(groups),)),
                pltpu.SemaphoreType.DMA((2 * len(payloads) + 2 * len(groups),)),
            ],
        ),
        compiler_params=pltpu.CompilerParams(dimension_semantics=("arbitrary",), vmem_limit_bytes=LIMIT),
        cost_estimate=pl.CostEstimate(
            flops=8 * height * tokens * model, bytes_accessed=8 * tokens * model, transcendentals=0
        ),
        name="backward_part",
    )(me, *toks, *cots, down, hidden, silu, slope, upg, upv, gtaps, vtaps)


def input_kernel(me_ref, *refs):
    count = (len(refs) - 3) // 2
    ggrads, vgrads = refs[:count], refs[count : 2 * count]
    gate_ref, value_ref, out_ref = refs[2 * count :]
    total = None
    for grads, weight_ref in ((ggrads, gate_ref), (vgrads, value_ref)):
        low = 0
        for ref in grads:
            high = low + ref.shape[0]
            term = lax.dot_general(
                ref[...], weight_ref[low:high], (((0,), (0,)), ((), ())), preferred_element_type=F32
            )
            total = term if total is None else total + term
            low = high
    out_ref[0] = total.astype(out_ref.dtype)


def input_part(me, ggrads, vgrads, gate_t, value_t, parts, odd, dtype):
    hidden, model = gate_t.shape
    tokens = ggrads[0].shape[1]
    rows, half = tokens // parts, parts // 2
    fields = [pl.BlockSpec((g.shape[0], rows), lambda i, me_ref: (0, me_ref[0] ^ (2 * i + odd))) for g in ggrads]
    weight = pl.BlockSpec((hidden, model), lambda i, me_ref: (0, 0))
    return pl.pallas_call(
        input_kernel,
        out_shape=jax.ShapeDtypeStruct((half, rows, model), dtype),
        grid_spec=pltpu.PrefetchScalarGridSpec(
            num_scalar_prefetch=1,
            grid=(half,),
            in_specs=fields * 2 + [weight, weight],
            out_specs=pl.BlockSpec((1, rows, model), lambda i, me_ref: (i, 0, 0)),
        ),
        compiler_params=pltpu.CompilerParams(dimension_semantics=("arbitrary",), vmem_limit_bytes=LIMIT),
        cost_estimate=pl.CostEstimate(
            flops=2 * hidden * tokens * model, bytes_accessed=2 * hidden * tokens + 3 * tokens * model, transcendentals=0
        ),
        name="input_part",
    )(me, *ggrads, *vgrads, gate_t, value_t)


def add(left, right, dtype):
    return (left.astype(F32) + right.astype(F32)).astype(dtype)


def reduce_chunk(sent, kept, first, second):
    got = exchange(sent, "rep", first)
    half = add(kept[1], got[1], BF16)
    over = exchange(half, "rep", second)
    mine = add(add(kept[0], got[0], F32), over, BF16)
    rest = [b for b in range(bit_count(lax.axis_size("rep"))) if b not in (first, second)]
    for at, bit in enumerate(rest):
        theirs = exchange(mine, "rep", bit)
        mine = add(mine, theirs, BF16 if at == len(rest) - 1 else F32)
    other = exchange(mine, "rep", second)
    pair = jnp.stack([mine, other])
    return pair, exchange(pair, "rep", first)


def place_kernel(scale, start, sides, swap, count, where_ref, *refs):
    pairs, refs = refs[: len(sides)], refs[len(sides) :]
    outs, (stage, out_sems) = refs[count : count + 3], refs[count + 3 :]
    height, size = stage.shape[2:]
    leaving = []
    for i, (pair, spot) in enumerate((pair.at[i], 2 * side + i) for pair, side in zip(pairs, sides) for i in range(2)):
        spot = ((spot >> 1) | ((spot & 1) << 1) if swap else spot) ^ where_ref[1]
        cols = pl.ds(pl.multiple_of(spot * size, size), size)
        for n, out_ref in enumerate(outs):
            stage[i, n] = pair[n * height : (n + 1) * height].astype(F32) * scale
            copy = pltpu.make_async_copy(stage.at[i, n], out_ref.at[pl.ds(start, height), cols], out_sems.at[i, n])
            copy.start()
            leaving.append(copy)
    for copy in leaving:
        copy.wait()


def place(start, height, sides, swap, where, pairs, outs, shape, scale):
    model = shape[1]
    anywhere = pl.BlockSpec(memory_space=pl.ANY)
    blocks = 2 * len(sides)
    return pl.pallas_call(
        functools.partial(place_kernel, scale, start, sides, swap, len(outs)),
        out_shape=(jax.ShapeDtypeStruct(shape, F32),) * 3,
        grid_spec=pltpu.PrefetchScalarGridSpec(
            num_scalar_prefetch=1,
            grid=(1,),
            in_specs=[pl.BlockSpec(memory_space=pltpu.VMEM)] * len(pairs) + [anywhere] * len(outs),
            out_specs=(anywhere,) * 3,
            scratch_shapes=[
                pltpu.VMEM((blocks, 3, height, model // 4), F32),
                pltpu.SemaphoreType.DMA((blocks, 3)),
            ],
        ),
        input_output_aliases={1 + len(pairs) + n: n for n in range(len(outs))},
        compiler_params=pltpu.CompilerParams(dimension_semantics=("arbitrary",), vmem_limit_bytes=LIMIT // 4),
        cost_estimate=pl.CostEstimate(
            flops=3 * height * model, bytes_accessed=9 * blocks // 2 * height * model, transcendentals=0
        ),
        name="place",
    )(where, *pairs, *outs)


def butterfly(value):
    for bit in range(bit_count(lax.axis_size("rep"))):
        value = value + exchange(value, "rep", bit)
    return value


def gather_relative(own):
    found = {0: own}
    base = bit_count(lax.axis_size("tp"))
    for bit in range(bit_count(lax.axis_size("fs"))):
        found.update({r | (1 << (base + bit)): exchange(item, "fs", bit) for r, item in list(found.items())})
    for bit in range(base):
        found.update({r | (1 << bit): exchange(item, "tp", bit) for r, item in list(found.items())})
    return [found[r] for r in range(len(found))]


def scatter_relative(sent, kept):
    moved = exchange(sent, "tp", 0)
    blocks = [add(kept[i], moved[i], F32) for i in range(kept.shape[0])]
    bits = [("tp", b) for b in range(1, bit_count(lax.axis_size("tp")))]
    bits += [("fs", b) for b in range(bit_count(lax.axis_size("fs")))]
    for axis, bit in bits:
        far = jnp.stack(blocks[1::2]).astype(BF16)
        moved = exchange(far, axis, bit)
        blocks = [add(item, moved[i], F32) for i, item in enumerate(blocks[0::2])]
    return blocks[0].astype(BF16)


def layer(tokens, cotangent, gate_weight, value_weight, down_weight, gate_taps, value_taps):
    rows, model = tokens.shape
    hidden = gate_weight.shape[1]
    parts = lax.axis_size("fs") * lax.axis_size("tp")
    scale = 1.0 / math.sqrt(rows * parts * lax.axis_size("rep"))
    me = (lax.axis_index("fs") * lax.axis_size("tp") + lax.axis_index("tp")).astype(jnp.int32)
    gate_t, value_t = gate_weight.T, value_weight.T
    gtaps, vtaps = gate_taps.T, value_taps.T
    where = jnp.stack([me, (2 * rep_bit(0) + rep_bit(1)).astype(jnp.int32)])

    cotangent, where, gtaps, vtaps = lax.optimization_barrier((cotangent, where, gtaps, vtaps))
    toks = gather_relative(tokens)
    cots = gather_relative(cotangent)
    fields = forward_part(where, toks, gate_t, value_t, gtaps, vtaps)
    ggrads, vgrads, sums, chunks = [], [], [], []
    groups = chunk_rows(hidden)
    for members in CALLS:
        mine = [groups[g] for g in members]
        found = backward_part(mine, where, toks, cots, down_weight, *fields, gtaps, vtaps)
        *payload, ggrad, vgrad = found[: len(found) - len(mine)]
        sums.extend(found[len(found) - len(mine) :])
        for start, _, heights, orders in mine:
            for height, order in zip(heights, orders):
                sent, kept, *payload = payload
                pairs = reduce_chunk(sent, kept, *order)
                chunks.append((start, height, order[0] == 1, pairs))
                start += height
        ggrads.append(ggrad)
        vgrads.append(vgrad)
    outs = ()
    for chunk, sides in FINISH:
        start, height, swap, pairs = chunks[chunk]
        picked = [pairs[side] for side in sides]
        outs = place(start, height, sides, swap, where, picked, outs, (hidden, model), scale)
    sums = butterfly(jnp.concatenate(sums, axis=1)) * scale
    away = input_part(where, ggrads, vgrads, gate_t, value_t, parts, 1, BF16)
    own = input_part(where, ggrads, vgrads, gate_t, value_t, parts, 0, F32)
    input_grad = scatter_relative(away, own)
    count = gate_taps.shape[0]
    return input_grad, outs[0].T, outs[1].T, outs[2], sums[:count], sums[count:]


def solution(mesh):
    in_specs = (
        P(("rep", "fs", "tp"), None),
        P(("rep", "fs", "tp"), None),
        P(None, ("fs", "tp")),
        P(None, ("fs", "tp")),
        P(("fs", "tp"), None),
        P(None, ("fs", "tp")),
        P(None, ("fs", "tp")),
    )
    out_specs = (
        P(("rep", "fs", "tp"), None),
        P(None, ("fs", "tp")),
        P(None, ("fs", "tp")),
        P(("fs", "tp"), None),
        P(None, ("fs", "tp")),
        P(None, ("fs", "tp")),
    )
    return jax.shard_map(layer, mesh=mesh, in_specs=in_specs, out_specs=out_specs, check_vma=False)
```
